32 devices in a mesh: rep: 2 (over x), fs: 8 (over z, y), tp: 2 (over core).
Axes of the slice: x: 2, y: 2, z: 4, core: 2. Of those that a mesh axis runs over, the one named last changes fastest.
Arguments:
- tokens: bfloat16 [4096, 2048], P(('rep', 'fs')), may hold values from -6 to 6
- mid_tokens: bfloat16 [4096, 2048], P(('rep', 'fs')), may hold values from -6 to 6
- out_grad: bfloat16 [4096, 2048], P(('rep', 'fs')), may hold values from -6 to 6
- gate_first: bfloat16 [2048, 3072], P('fs', 'tp'), may hold values from -0.125 to 0.125
- up_first: bfloat16 [2048, 3072], P('fs', 'tp'), may hold values from -0.125 to 0.125
- down_first: bfloat16 [3072, 2048], P('tp', 'fs'), may hold values from -0.109375 to 0.109375
- gate_second: bfloat16 [2048, 3072], P('fs', 'tp'), may hold values from -0.125 to 0.125
- up_second: bfloat16 [2048, 3072], P('fs', 'tp'), may hold values from -0.125 to 0.125
- down_second: bfloat16 [3072, 2048], P('tp', 'fs'), may hold values from -0.109375 to 0.109375
Outputs:
- input_grad: bfloat16 [4096, 2048], P(('rep', 'fs'))
- down_grad: float32 [3072, 2048], P('tp', 'fs')
- row_norms: float32 [3072], P('tp')
The draws below stay inside these ranges and needn't reach their ends.
All inputs are finite; a program needn't handle non-finite values.
Results may differ from the reference program's by a relative error of at most 0.025.
Values may be sent and summed in bfloat16 or wider, within the bound.
A program may use at most 128 MiB of HBM per device.

```python
import jax
import jax.numpy as jnp
from jax import lax

D = 2048
FF = 3072
TOKENS = 4096
N_TP = 2


def strengthened(array, stream_key, source, target, parts, factor):
    def block_of(position):
        return (jnp.arange(array.shape[position]) // (array.shape[position] // parts)).reshape((-1,) + (1,) * (array.ndim - 1 - position))

    first = jax.random.permutation(stream_key, parts)[block_of(target)]
    other_side = (block_of(target) + parts // 2) % parts
    return jnp.where((block_of(source) == first) | (block_of(source) == other_side), factor * array, array)


def level_of(own_key, shape, cuts, smallest, high):
    loudness = 1.0
    for dim, parts in cuts:
        draws = jax.random.uniform(jax.random.fold_in(jax.random.fold_in(own_key, 6), dim), (parts,), jnp.float32, smallest / len(cuts), high / len(cuts))
        loudness = loudness * jnp.repeat(jnp.exp(draws), shape[dim] // parts).reshape((-1,) + (1,) * (len(shape) - 1 - dim))
    return loudness


def gaussian(stream_key, shape, deviation, most, cuts=(), held_as=jnp.bfloat16):
    values = jax.random.normal(stream_key, shape, jnp.float32) * deviation
    if len(cuts) > 0:
        values = level_of(stream_key, shape, cuts, -0.22, 0.18) * values
    return jnp.clip(values, min=-most, max=most).astype(held_as)


def noise_with(rng, shape, scale, most, pieces, heavy, kind=jnp.bfloat16):
    values = scale * jax.random.normal(rng, shape, jnp.float32)
    if pieces:
        values = values * level_of(rng, shape, pieces, -0.22, 0.18)
    return jnp.clip(strengthened(values, jax.random.fold_in(rng, 3), *heavy), -most, most).astype(kind)


def setup_inputs(seed: int = 0) -> dict:
    arg_keys = jax.random.split(jax.random.key(seed), 10)
    return {
        "tokens": gaussian(arg_keys[0], (TOKENS, D), 1.0, 6.0, ((0, 16),)),
        "mid_tokens": gaussian(arg_keys[1], (TOKENS, D), 1.0, 6.0, ((0, 16),)),
        "out_grad": noise_with(arg_keys[2], (TOKENS, D), 1.0, 6.0, ((0, 16),), (0, 1, 16, 2.0)),
        "gate_first": gaussian(arg_keys[3], (D, FF), D ** -0.5, 0.125, ((0, 8), (1, 2))),
        "up_first": gaussian(arg_keys[4], (D, FF), D ** -0.5, 0.125, ((0, 8), (1, 2))),
        "down_first": gaussian(arg_keys[5], (FF, D), FF ** -0.5, 0.109375, ((0, 2), (1, 8))),
        "gate_second": gaussian(arg_keys[6], (D, FF), D ** -0.5, 0.125, ((0, 8), (1, 2))),
        "up_second": gaussian(arg_keys[7], (D, FF), D ** -0.5, 0.125, ((0, 8), (1, 2))),
        "down_second": gaussian(arg_keys[8], (FF, D), FF ** -0.5, 0.109375, ((0, 2), (1, 8))),
    }


eps = 1e-06

def split_partials(d_gate, d_up, gate_w, up_w):
    width = d_gate.shape[1] // N_TP
    total = jnp.zeros((d_gate.shape[0], gate_w.shape[0]), jnp.float32)
    dims = (((1,), (1,)), ((), ()))
    for block in range(N_TP):
        lower = block * width
        part = lax.dot_general(d_gate[:, lower:lower + width], gate_w[:, lower:lower + width], dims, preferred_element_type=jnp.float32)
        part = part + lax.dot_general(d_up[:, lower:lower + width], up_w[:, lower:lower + width], dims, preferred_element_type=jnp.float32)
        rounded = lax.optimization_barrier(part.astype(jnp.bfloat16))
        total = total + rounded.astype(jnp.float32)
    return total

def half_back(field, carried, gate_w, up_w, down_w):
    scale = lax.rsqrt(lax.optimization_barrier(jnp.mean(field * field, axis=1, keepdims=True)) + eps)
    normed = field * scale
    normed_b = normed.astype(jnp.bfloat16)
    gate = jnp.dot(normed_b, gate_w, preferred_element_type=jnp.float32)
    upper = jnp.dot(normed_b, up_w, preferred_element_type=jnp.float32)
    back = 0.5 * lax.dot_general(carried, down_w, (((1,), (1,)), ((), ())), preferred_element_type=jnp.float32)
    logistic = jax.nn.sigmoid(gate)
    activated = gate * logistic
    hidden = (activated * upper).astype(jnp.bfloat16)
    d_gate = (back * upper * logistic * (1.0 + gate * (1.0 - logistic))).astype(jnp.bfloat16)
    d_up = (back * activated).astype(jnp.bfloat16)
    d_normed = split_partials(d_gate, d_up, gate_w, up_w)
    d_field = carried.astype(jnp.float32) + scale * (d_normed - normed * lax.optimization_barrier(jnp.mean(d_normed * normed, axis=1, keepdims=True)))
    return (d_field, hidden)

def reference(tokens, mid_tokens, out_grad, gate_first, up_first, down_first, gate_second, up_second, down_second):
    d_mid, unused = half_back(mid_tokens.astype(jnp.float32), out_grad, gate_second, up_second, down_second)
    mid_grad = d_mid.astype(jnp.bfloat16)
    d_input, hidden = half_back(tokens.astype(jnp.float32), mid_grad, gate_first, up_first, down_first)
    down_grad = 0.5 * lax.dot_general(hidden, mid_grad, (((0,), (0,)), ((), ())), preferred_element_type=jnp.float32)
    row_norms = lax.optimization_barrier(jnp.sum(down_grad * down_grad, axis=1))
    return (d_input.astype(jnp.bfloat16), down_grad, row_norms)
```

```python
import functools

import jax
import jax.numpy as jnp
from jax import lax
from jax.experimental import pallas as pl
from jax.experimental.pallas import tpu as pltpu
from jax.sharding import PartitionSpec as P

eps = 1e-06
f32, bf16 = jnp.float32, jnp.bfloat16


def kernel(sizes, tok, mid, cot, g1, u1, v1, g2, u2, v2, out, grad, norms, full1, downs1, full2, downs2, toks, mids, cots, mgs, xb, hidden, d_gate, d_up, mgt, gates, uppers, part, got1, snd2, got2, dn, rs_out, rs_in, gb, nb, w_send, w_recv, own_sem, x_send, x_recv, s1_send, s1_recv, s2_send, s2_recv, s3_send, s3_recv, r_send, r_recv, g_send, g_recv, n_send, n_recv):
    R, F, T, n, D, H, pieces = sizes
    S, half, C, width = D // F, D // F // 2, D // T, H // pieces
    both = 2 if pieces > 1 else 1
    r, f, t = (lax.axis_index(a) for a in ("rep", "fs", "tp"))

    def fs_at(position):
        q = lax.rem(position + 2 * F, F)
        hi = q // (F // 2)
        return (1 - hi) * 2 * q + hi * (2 * (F - 1 - q) + 1)

    odd = lax.rem(f, 2)
    p = (1 - odd) * (f // 2) + odd * (F - 1 - f // 2)
    side = (fs_at(p + 1), fs_at(p - 1))

    barrier = pltpu.get_barrier_semaphore()
    for axis, size, me in (("rep", R, r), ("fs", F, f), ("tp", T, t)):
        for k in range(1, size):
            pl.semaphore_signal(barrier, inc=1, device_id={axis: lax.rem(me + k, size)}, device_id_type=pl.DeviceIdType.MESH)
    pl.semaphore_wait(barrier, R + F + T - 3)

    def remote(src, dst, send, recv, **where):
        return pltpu.make_async_remote_copy(src_ref=src, dst_ref=dst, send_sem=send, recv_sem=recv, device_id=where, device_id_type=pl.DeviceIdType.MESH)

    fulls = ((full1, downs1), (full2, downs2))

    second_gu, second_d = (1, 0, both, 2 * H // both, 0), (1, 1, pieces, width, both)
    first_gu, first_d = (0,) + second_gu[1:], (0,) + second_d[1:]

    def ring(phase, d, distance, step, piece):
        b, which, count, wide, sem = phase
        owner = fs_at(p - distance if d == 0 else p + distance)
        rows = pl.ds(pl.multiple_of(owner * S + d * half, half), half)
        ref = fulls[b][which].at[rows]
        if count > 1:
            ref = fulls[b][which].at[rows, pl.ds(pl.multiple_of(piece * wide, 128), wide)]
        return remote(ref, ref, w_send.at[b, which, d], w_recv.at[b, d, step, sem + piece], fs=side[d])

    def start_ring(phase):
        for piece in range(phase[2]):
            for d in (0, 1):
                ring(phase, d, 0, 0, piece).start()

    def serve(phase, lo, hi, of):
        relays = (F - 2) * phase[2]

        @pl.loop(relays * lo // of, relays * hi // of)
        def _(k):
            step, piece = k // phase[2], lax.rem(k, phase[2])
            for d in (0, 1):
                ring(phase, d, step + 1, step, piece).wait_recv()
                ring(phase, d, step + 1, step + 1, piece).start()

    def end_ring(phase):
        for piece in range(phase[2]):
            for d in (0, 1):
                ring(phase, d, F - 1, F - 2, piece).wait_recv()

    def drain(b):
        for which in (0, 1):
            whole = fulls[b][which].at[pl.ds(0, (F - 1) * half)]
            for d in (0, 1):
                remote(whole, whole, w_send.at[b, which, d], w_recv.at[b, d, 0, 0], fs=side[d]).wait_send()

    mine = pl.ds(pl.multiple_of(r * n, n), n)
    pairs = (mids, cots, toks, mgs)
    held = pl.ds(pl.multiple_of(f * S, S), S)
    def pair_loads(g, u, full):
        if H % 128 > 0:
            return [(g, full.at[held])]
        taken = pl.ds(pl.multiple_of(r * H, 128), H)
        return [(g.at[:, taken], full.at[held, pl.ds(0, H)]), (u.at[:, taken], full.at[held, pl.ds(H, H)])]

    wanted = pair_loads(g2, u2, full2)
    ahead = len(wanted)
    wanted += [(mid, mids.at[mine]), (cot, cots.at[mine]), (tok, toks.at[mine]), (v2, downs2.at[held]), (v1, downs1.at[held])]
    wanted += pair_loads(g1, u1, full1)
    loads = [pltpu.make_async_copy(src, dst, own_sem.at[i]) for i, (src, dst) in enumerate(wanted)]
    for c in loads:
        c.start()

    def swap(i):
        return [remote(pairs[i].at[mine], pairs[i].at[mine], x_send.at[i, k - 1], x_recv.at[i, k - 1], rep=lax.rem(r + k, R)) for k in range(1, R)]

    def swap_in(i):
        for k in range(1, R):
            rows = pl.ds(pl.multiple_of(lax.rem(r + R - k, R) * n, n), n)
            remote(pairs[i].at[rows], pairs[i].at[rows], x_send.at[i, k - 1], x_recv.at[i, k - 1], rep=lax.rem(r + k, R)).wait_recv()

    for c in loads[:ahead]:
        c.wait()
    start_ring(second_gu)
    for i in range(3):
        loads[ahead + i].wait()
        for c in swap(i):
            c.start()
    for c in loads[ahead + 3 :]:
        c.wait()

    def normalise(pair):
        @pl.loop(0, R * n // 32)
        def _(i):
            rows = pl.ds(pl.multiple_of(i * 32, 32), 32)
            u = pair[rows, :].astype(f32)
            xb[rows, :] = (u * lax.rsqrt(jnp.mean(u * u, axis=1, keepdims=True) + eps)).astype(bf16)

    chunk = 256 if H % 256 == 0 else 128 if H % 128 == 0 else H

    def cols(which, j):
        if chunk == H:
            return pl.ds(which * H, H)
        return pl.ds(pl.multiple_of(which * H + j * chunk, 128), chunk)

    def forward(full):
        @pl.loop(0, H // chunk)
        def _(j):
            gate = jnp.dot(xb[...], full[:, cols(0, j)], preferred_element_type=f32)
            upper = jnp.dot(xb[...], full[:, cols(1, j)], preferred_element_type=f32)
            hidden[:, cols(0, j)] = (gate * jax.nn.sigmoid(gate) * upper).astype(bf16)
            gates[:, cols(0, j)] = gate
            uppers[:, cols(0, j)] = upper

    def backed(downs, c_ref):
        @pl.loop(0, H // chunk)
        def _(j):
            gate, upper = gates[:, cols(0, j)], uppers[:, cols(0, j)]
            back = 0.5 * jnp.dot(c_ref[...], downs[:, cols(0, j)], preferred_element_type=f32)
            logistic = jax.nn.sigmoid(gate)
            d_gate[:, cols(0, j)] = (back * upper * logistic * (1.0 + gate * (1.0 - logistic))).astype(bf16)
            d_up[:, cols(0, j)] = (back * gate * logistic).astype(bf16)

    dims = (((1,), (1,)), ((), ()))

    def backward(full, lo, hi):
        @pl.loop(lo, hi)
        def _(j):
            rows = pl.ds(pl.multiple_of(j * 256, 256), 256)
            total = lax.dot_general(d_gate[...], full[rows, 0:H], dims, preferred_element_type=f32)
            total = total + lax.dot_general(d_up[...], full[rows, H : 2 * H], dims, preferred_element_type=f32)
            part[:, rows] = total.astype(bf16)

    def block_of(k):
        return pl.ds(pl.multiple_of(k * C, 128), C)

    def stage1(b):
        return [remote(part.at[:, block_of(lax.rem(t + k, T))], got1.at[b, k - 1], s1_send.at[b, k - 1], s1_recv.at[b, k - 1], tp=lax.rem(t + k, T)) for k in range(1, T)]

    def stage2(b):
        return [remote(snd2.at[k - 1], got2.at[b, k - 1], s2_send.at[b, k - 1], s2_recv.at[b, k - 1], rep=lax.rem(r + k, R)) for k in range(1, R)]

    def stage3(b, owner):
        ref = dn.at[b, :, block_of(owner)]
        return lambda k: remote(ref, ref, s3_send.at[b, k - 1], s3_recv.at[b, k - 1], tp=lax.rem(t + k, T))

    def summed(b, base, i):
        rows = pl.ds(pl.multiple_of(base * n + i * 32, 32), 32)
        total = part[rows, block_of(t)].astype(f32)
        for k in range(T - 1):
            total = total + got1[b, k, rows, :].astype(f32)
        return total

    def reduce_tp(b):
        for c in stage1(b):
            c.wait()
        for k in range(1, R):
            @pl.loop(0, n // 32)
            def _(i, k=k):
                snd2[k - 1, pl.ds(pl.multiple_of(i * 32, 32), 32), :] = summed(b, lax.rem(r + k, R), i).astype(bf16)
        for c in stage2(b):
            c.start()

    def reduce_rep(b):
        for c in stage2(b):
            c.wait()

        @pl.loop(0, n // 32)
        def _(i):
            rows = pl.ds(pl.multiple_of(i * 32, 32), 32)
            total = summed(b, r, i)
            for k in range(R - 1):
                total = total + got2[b, k, rows, :].astype(f32)
            dn[b, rows, block_of(t)] = total.astype(bf16)

        for k in range(1, T):
            stage3(b, t)(k).start()

    def finish(b, pair, carried, result, offset):
        for k in range(1, T):
            stage3(b, lax.rem(t + T - k, T))(k).wait_recv()
            stage3(b, t)(k).wait_send()

        @pl.loop(0, n // 32)
        def _(i):
            rows = pl.ds(pl.multiple_of(i * 32, 32), 32)
            wide = pl.ds(pl.multiple_of(r * n + i * 32, 32), 32)
            u = pair[wide, :].astype(f32)
            scale = lax.rsqrt(jnp.mean(u * u, axis=1, keepdims=True) + eps)
            normed = u * scale
            d = dn[b, rows, :].astype(f32)
            d_u = carried[wide, :].astype(f32) + scale * (d - normed * jnp.mean(d * normed, axis=1, keepdims=True))
            result[pl.ds(pl.multiple_of(offset + i * 32, 32), 32), :] = d_u.astype(bf16)

    serve(second_gu, 0, 10, 12)
    swap_in(0)
    normalise(mids)
    serve(second_gu, 10, 12, 12)
    start_ring(second_d)
    end_ring(second_gu)
    serve(second_d, 0, 3, 18)
    forward(full2)
    serve(second_d, 3, 18, 18)
    start_ring(first_gu)
    swap_in(1)
    end_ring(second_d)
    backed(downs2, cots)
    serve(first_gu, 0, 1, 12)
    backward(full2, 0, D // 512)
    serve(first_gu, 1, 2, 12)
    backward(full2, D // 512, D // 256)
    for c in stage1(1):
        c.start()
    serve(first_gu, 2, 3, 12)
    reduce_tp(1)
    serve(first_gu, 3, 4, 12)
    swap_in(2)
    normalise(toks)
    serve(first_gu, 4, 6, 12)
    reduce_rep(1)
    serve(first_gu, 6, 7, 12)
    finish(1, mids, cots, mgs, r * n)
    for c in swap(3):
        c.start()
    serve(first_gu, 7, 12, 12)
    start_ring(first_d)
    end_ring(first_gu)

    forward(full1)
    serve(first_d, 0, 6, 18)
    swap_in(3)

    @pl.loop(0, D // 256)
    def _(j):
        part_cols = pl.ds(pl.multiple_of(j * 256, 256), 256)
        mgt[part_cols, :] = mgs[:, part_cols].T

    serve(first_d, 6, 18, 18)

    def strip(piece):
        return pl.ds(pl.multiple_of(piece * width, 128), width) if pieces > 1 else slice(None)

    def product(d, position, piece):
        rows = pl.ds(pl.multiple_of(fs_at(position) * S + d * half, half), half)
        return 0.5 * jnp.dot(mgt[rows, :], hidden[:, strip(piece)], preferred_element_type=f32)

    def view(ref, piece):
        return ref.at[:, strip(piece)] if pieces > 1 else ref

    def rs(d, s, piece):
        return remote(view(rs_out.at[d, s], piece), view(rs_in.at[d, s], piece), r_send.at[d, s, piece], r_recv.at[d, s, piece], fs=side[d])

    def passed(lo, hi):
        @pl.loop(1 + (F - 2) * lo // 6, 1 + (F - 2) * hi // 6)
        def _(s):
            for piece in range(pieces):
                for d in (0, 1):
                    value = product(d, p - 1 - s if d == 0 else p + 1 + s, piece)
                    rs(d, s - 1, piece).wait_recv()
                    rs_out[d, s, :, strip(piece)] = (value + rs_in[d, s - 1, :, strip(piece)].astype(f32)).astype(bf16)
                    rs(d, s, piece).start()

    for piece in range(pieces):
        for d in (0, 1):
            rs_out[d, 0, :, strip(piece)] = product(d, p - 1 if d == 0 else p + 1, piece).astype(bf16)
            rs(d, 0, piece).start()
    end_ring(first_d)
    backed(downs1, mgs)
    passed(0, 1)
    backward(full1, 0, D // 512)
    passed(1, 2)
    backward(full1, D // 512, D // 256)
    for c in stage1(0):
        c.start()
    passed(2, 3)
    reduce_tp(0)
    passed(3, 6)

    def trade(owner, piece):
        ref = view(gb.at[owner], piece)
        return lambda k: remote(ref, ref, g_send.at[k - 1, piece], g_recv.at[k - 1, piece], rep=lax.rem(r + k, R))

    for piece in range(pieces):
        for d in (0, 1):
            value = product(d, p, piece)
            rs(d, F - 2, piece).wait_recv()
            gb[r, pl.ds(d * half, half), strip(piece)] = (value + rs_in[d, F - 2, :, strip(piece)].astype(f32)).astype(bf16)
        for k in range(1, R):
            trade(r, piece)(k).start()
    reduce_rep(0)
    finish(0, toks, mgs, out, 0)
    for piece in range(pieces):
        for k in range(1, R):
            trade(lax.rem(r + R - k, R), piece)(k).wait_recv()
            trade(r, piece)(k).wait_send()
    for k in range(R):
        g = gb[k].astype(f32)
        grad[:, k * H : (k + 1) * H] = g
        nb[f, :, k * H : (k + 1) * H] = jnp.sum(g * g, axis=0, keepdims=True)

    def tell(owner):
        return lambda k: remote(nb.at[owner], nb.at[owner], n_send.at[k - 1], n_recv.at[k - 1], fs=lax.rem(f + k, F))

    for k in range(1, F):
        tell(f)(k).start()
    for b in (0, 1):
        drain(b)
    for i in range(4):
        for c in swap(i):
            c.wait_send()

    @pl.loop(0, F - 1)
    def _(s):
        for piece in range(pieces):
            for d in (0, 1):
                rs(d, s, piece).wait_send()

    for k in range(1, F):
        tell(lax.rem(f + F - k, F))(k).wait_recv()
        tell(f)(k).wait_send()
    total = nb[0]
    for k in range(1, F):
        total = total + nb[k]
    norms[...] = total


def on_device(sizes, tokens, mid_tokens, out_grad, gate_first, up_first, down_first, gate_second, up_second, down_second):
    R, F, T, n, D, H, pieces = sizes
    S, half = D // F, D // F // 2
    start = lax.axis_index("rep") * H

    def own(gate_w, up_w, down_w):
        down = lax.dynamic_slice_in_dim(down_w, start, H, 0).T
        if H % 128 == 0:
            return gate_w, up_w, down
        pair = [lax.dynamic_slice_in_dim(w, start, H, 1) for w in (gate_w, up_w)]
        return jnp.concatenate(pair, axis=1), up_w, down

    dma = pltpu.SemaphoreType.DMA
    m = R * n
    any_space = pl.BlockSpec(memory_space=pl.ANY)
    vmem = pl.BlockSpec(memory_space=pltpu.VMEM)
    d_input, grad, norms = pl.pallas_call(
        functools.partial(kernel, sizes),
        out_shape=(
            jax.ShapeDtypeStruct((n, D), bf16),
            jax.ShapeDtypeStruct((S, R * H), f32),
            jax.ShapeDtypeStruct((1, R * H), f32),
        ),
        in_specs=[any_space] * 9,
        out_specs=(vmem, vmem, vmem),
        scratch_shapes=[
            pltpu.VMEM((D, 2 * H), bf16),
            pltpu.VMEM((D, H), bf16),
            pltpu.VMEM((D, 2 * H), bf16),
            pltpu.VMEM((D, H), bf16),
            pltpu.VMEM((m, D), bf16),
            pltpu.VMEM((m, D), bf16),
            pltpu.VMEM((m, D), bf16),
            pltpu.VMEM((m, D), bf16),
            pltpu.VMEM((m, D), bf16),
            pltpu.VMEM((m, H), bf16),
            pltpu.VMEM((m, H), bf16),
            pltpu.VMEM((m, H), bf16),
            pltpu.VMEM((D, m), bf16),
            pltpu.VMEM((m, H), f32),
            pltpu.VMEM((m, H), f32),
            pltpu.VMEM((m, D), bf16),
            pltpu.VMEM((2, T - 1, m, D // T), bf16),
            pltpu.VMEM((R - 1, n, D // T), bf16),
            pltpu.VMEM((2, R - 1, n, D // T), bf16),
            pltpu.VMEM((2, n, D), bf16),
            pltpu.VMEM((2, F - 1, half, H), bf16),
            pltpu.VMEM((2, F - 1, half, H), bf16),
            pltpu.VMEM((R, S, H), bf16),
            pltpu.VMEM((F, 1, R * H), f32),
            dma((2, 2, 2)),
            dma((2, 2, F - 1, pieces + (2 if pieces > 1 else 1))),
            dma((9,)),
            dma((4, R - 1)),
            dma((4, R - 1)),
            dma((2, T - 1)),
            dma((2, T - 1)),
            dma((2, R - 1)),
            dma((2, R - 1)),
            dma((2, T - 1)),
            dma((2, T - 1)),
            dma((2, F - 1, pieces)),
            dma((2, F - 1, pieces)),
            dma((R - 1, pieces)),
            dma((R - 1, pieces)),
            dma((F - 1,)),
            dma((F - 1,)),
        ],
        compiler_params=pltpu.CompilerParams(
            collective_id=0, has_side_effects=True, vmem_limit_bytes=67043328
        ),
    )(
        tokens,
        mid_tokens,
        out_grad,
        *own(gate_first, up_first, down_first),
        *own(gate_second, up_second, down_second),
    )
    return d_input, grad.T, norms.reshape(-1)


def square_kernel(sizes, tok, mid, cot, g1, u1, v1, g2, u2, v2, out, grad, norms, gu, dd, acts, xb, acc, bk, dg, hT, part, sib, xs, xr, zs, zr, dbuf, scb, ps, pr, obs, obr, gys, gyr, g2s, g2r, gzs, gq, nb, own_sem, wz_send, wz_recv, wy_send, wy_recv, a_send, a_recv, s_send, s_recv, x_send, x_recv, z_send, z_recv, p_send, p_recv, o_send, o_recv, gy_send, gy_recv, g2_send, g2_recv, gz_send, gz_recv, gx_send, gx_recv, n_send, n_recv):
    R, F, T, n, D, H = sizes
    S, half, h = D // F, D // 2, n // 2
    r, f, t = (lax.axis_index(a) for a in ("rep", "fs", "tp"))
    z, y = f // 2, lax.rem(f, 2)
    zl, zh = lax.rem(z, 2), z // 2

    def fs_of(k, side):
        return 2 * (2 * lax.rem(zh + k // 2, 2) + lax.rem(zl + k % 2, 2)) + side

    to_x, to_y, to_s = {"rep": 1 - r}, {"fs": fs_of(0, 1 - y)}, {"tp": 1 - t}
    to_z = [None] + [{"fs": fs_of(k, y)} for k in (1, 2, 3)]
    inn = lax.rem(zl + zh, 2)
    inner, outer = inn == 1, inn == 0
    me, jx, jz, jd = 2 * r + zl, 2 * (1 - r) + zl, 2 * r + 1 - zl, 2 * (1 - r) + 1 - zl

    barrier = pltpu.get_barrier_semaphore()
    for axis, size, at in (("rep", R, r), ("fs", F, f), ("tp", T, t)):
        for k in range(1, size):
            pl.semaphore_signal(barrier, inc=1, device_id={axis: lax.rem(at + k, size)}, device_id_type=pl.DeviceIdType.MESH)

    def at(start, size, step=8):
        return pl.ds(pl.multiple_of(start, step), size)

    def remote(src, dst, send, recv, where):
        return pltpu.make_async_remote_copy(src_ref=src, dst_ref=dst, send_sem=send, recv_sem=recv, device_id=where, device_id_type=pl.DeviceIdType.MESH)

    weights = ((g1, u1, v1), (g2, u2, v2))
    fields = (mid, cot, tok)

    def source(b, p, q):
        ref = weights[b][p]
        return ref.at[at(q * H, H)] if p == 2 else ref.at[:, at(q * H, H, 128)]

    def place(b, p, owner):
        if p == 2:
            return dd.at[b, :, at(owner * S, S, 128)]
        return gu.at[b, at(owner * S, S), pl.ds(p * H, H)]

    loads = {}
    for i in range(3):
        loads["a", i] = pltpu.make_async_copy(fields[i], acts.at[i, at(me * n, n)], own_sem.at[i])
    for b in (1, 0):
        for p in range(3):
            loads["w", b, p] = pltpu.make_async_copy(source(b, p, me), place(b, p, f), own_sem.at[3 + 3 * b + p])
    for c in loads.values():
        c.start()
    pl.semaphore_wait(barrier, R + F + T - 3)

    def w_first(b, p, k):
        q = me if k == 2 else jz
        return remote(source(b, p, q), place(b, p, f), wz_send.at[b, p, k], wz_recv.at[b, p, k], to_z[k])

    def w_relay(b, p):
        ref = place(b, p, fs_of(1, y))
        return remote(ref, ref, wz_send.at[b, p, 0], wz_recv.at[b, p, 3], to_z[2])

    def w_cross(b, p, k):
        ref = place(b, p, fs_of(k, y))
        return remote(source(b, p, me) if isinstance(k, int) and k == 0 else ref, ref, wy_send.at[b, p, k], wy_recv.at[b, p, k], to_y)

    def w_arrived(b, p, k):
        ref = place(b, p, fs_of(k, y))
        remote(ref, ref, wz_send.at[b, p, k], wz_recv.at[b, p, k], to_z[1]).wait_recv()

    def crossed(b, pieces, k):
        for p in pieces:
            ref = place(b, p, fs_of(k, 1 - y))
            remote(ref, ref, wy_send.at[b, p, k], wy_recv.at[b, p, k], to_y).wait_recv()

    def serve(b, pieces, k, near=False):
        for p in pieces:
            w_arrived(b, p, k)
            if near:
                @pl.when(inner)
                def _(p=p):
                    w_relay(b, p).start()
            w_cross(b, p, k).start()

    mine, other = at(t * half, half, 128), at((1 - t) * half, half, 128)

    def rows_of(j):
        return at(j * n, n)

    def a_copy(i, kind):
        if kind < 2:
            dst = acts.at[i, rows_of(me), mine]
            return remote(fields[i].at[:, mine] if i < 3 else dst, dst, a_send.at[i, kind], a_recv.at[i, kind], (to_z[1], to_x)[kind])
        ref = acts.at[i, rows_of({2: jz, 3: jz, 4: jx, 5: jd, 6: me}[kind]), mine]
        return remote(ref, ref, a_send.at[i, kind], a_recv.at[i, kind], to_x if kind == 2 else to_s)

    def a_arrived(i, kind):
        j = (jz, jx, jd, jz, jx, jd, me)[kind]
        ref = acts.at[i, rows_of(j), mine if kind < 3 else other]
        remote(ref, ref, a_send.at[i, kind], a_recv.at[i, kind], to_x).wait_recv()

    def a_zn(i):
        a_arrived(i, 0)
        a_copy(i, 2).start()
        a_copy(i, 3).start()

    def a_x(i):
        a_arrived(i, 1)
        a_copy(i, 4).start()

    def a_d(i):
        a_arrived(i, 2)
        a_copy(i, 5).start()

    def a_s(i):
        for kind in (3, 4, 5) + ((6,) if i == 3 else ()):
            a_arrived(i, kind)

    def normalise(i, lo, hi):
        @pl.loop(lo * n // 32, hi * n // 32)
        def _(c):
            rows = at(c * 32, 32)
            u = acts[i, rows, :].astype(f32)
            xb[rows, :] = (u * lax.rsqrt(jnp.mean(u * u, axis=1, keepdims=True) + eps)).astype(bf16)

    nt = (((1,), (1,)), ((), ()))

    def forward(b, owner, first=False):
        cut = at(owner * S, S, 128)

        @pl.loop(0, 2 * H // 256)
        def _(j):
            cols = at(j * 256, 256, 128)
            value = jnp.dot(xb[:, cut], gu[b, at(owner * S, S), cols], preferred_element_type=f32)
            acc[:, cols] = value if first else acc[:, cols] + value

    def backed(b, i, owner, first=False):
        cut = at(owner * S, S, 128)

        @pl.loop(0, 2)
        def _(j):
            rows = at(j * 2 * n, 2 * n)
            value = lax.dot_general(acts[i, rows, cut], dd[b, :, cut], nt, preferred_element_type=f32)
            bk[rows, :] = value if first else bk[rows, :] + value

    def hidden():
        @pl.loop(0, 4 * n // 128)
        def _(c):
            rows = at(c * 128, 128)
            gate = acc[rows, 0:H]
            hT[:, at(c * 128, 128, 128)] = (gate * jax.nn.sigmoid(gate) * acc[rows, H : 2 * H]).astype(bf16).T

    def elementwise():
        @pl.loop(0, 4 * n // 64)
        def _(c):
            rows = at(c * 64, 64)
            gate, upper, back = acc[rows, 0:H], acc[rows, H : 2 * H], 0.5 * bk[rows, :]
            logistic = jax.nn.sigmoid(gate)
            dg[rows, 0:H] = (back * upper * logistic * (1.0 + gate * (1.0 - logistic))).astype(bf16)
            dg[rows, H : 2 * H] = (back * gate * logistic).astype(bf16)

    def partial(b, side, c):
        rows = at(side * 2 * n, 2 * n)

        @pl.loop(0, half // 256)
        def _(j):
            wide = c * half + j * 256
            total = lax.dot_general(dg[rows, :], gu[b, at(wide, 256), :], nt, preferred_element_type=f32)
            part[rows, at(wide, 256, 128)] = total.astype(bf16)

    def sibling(b, i, side):
        rows = at(side * 2 * n, 2 * n)
        return remote(part.at[rows, other], sib.at[b, rows], s_send.at[b, i], s_recv.at[b, i], to_s)

    def partials(b, between=None):
        for i, side in enumerate((1 - r, r)):
            partial(b, side, 1 - t)
            sibling(b, i, side).start()
            partial(b, side, t)
            if between is not None:
                between(i)

    def x_copy(b, piece):
        rows = pl.ds(piece * h, h)
        return remote(xs.at[rows], xr.at[b, rows], x_send.at[b, piece], x_recv.at[b, piece], to_x)

    def z_copy(b, piece):
        rows = pl.ds(piece * h, h)
        return remote(zs.at[rows], zr.at[b, rows], z_send.at[b, piece], z_recv.at[b, piece], to_z[1])

    def own_sum(b, rows):
        return part[rows, mine].astype(f32) + sib[b, rows, :].astype(f32)

    def x_step(b):
        sibling(b, 0, 1 - r).wait_recv()
        for piece in range(4):
            base = (jd if piece < 2 else jx) * n + (piece % 2) * h

            @pl.loop(0, h // 32)
            def _(c, base=base, piece=piece):
                xs[at(piece * h + c * 32, 32), :] = own_sum(b, at(base + c * 32, 32)).astype(bf16)

            x_copy(b, piece).start()
        sibling(b, 1, r).wait_recv()

    def z_step(b, piece):
        x_copy(b, piece).wait_recv()

        @pl.loop(0, h // 32)
        def _(c):
            rows = at(piece * h + c * 32, 32)
            total = own_sum(b, at(jz * n + piece * h + c * 32, 32)) + xr[b, rows, :].astype(f32)
            zs[rows, :] = total.astype(bf16)

        z_copy(b, piece).start()

    def sum_send(b, buf, piece, base, extra, copy):
        @pl.loop(0, h // 32)
        def _(c):
            total = own_sum(b, at(base + c * 32, 32))
            if extra is not None:
                total = total + extra[b, at(c * 32, 32), :].astype(f32)
            buf[at(piece * h + c * 32, 32), :] = total.astype(bf16)

        copy(b, piece).start()

    def spread(i):
        sibling(0, i, (1 - r, r)[i]).wait_recv()
        if i == 0:
            sum_send(0, xs, 0, jd * n, None, x_copy)
            sum_send(0, zs, 0, jd * n + h, None, z_copy)
            sum_send(0, xs, 1, jx * n, None, x_copy)
        else:
            sum_send(0, zs, 1, jz * n + h, None, z_copy)

    def spread_end():
        x_copy(0, 0).wait_recv()
        sum_send(0, zs, 2, jz * n, xr, z_copy)
        z_copy(0, 0).wait_recv()
        sum_send(0, xs, 2, jx * n + h, zr, x_copy)

    def finish(b, ui, ci, parts, store):
        for piece, (px, pz) in enumerate(parts):
            x_copy(b, px).wait_recv()
            z_copy(b, pz).wait_recv()

            @pl.loop(piece * h // 32, (piece + 1) * h // 32)
            def _(c, piece=piece, px=px, pz=pz):
                rows, wide = at(c * 32, 32), at(me * n + c * 32, 32)
                from_x, from_z = (at((q - piece) * h + c * 32, 32) for q in (px, pz))
                d = own_sum(b, wide) + xr[b, from_x, :].astype(f32) + zr[b, from_z, :].astype(f32)
                u = acts[ui, wide, :].astype(f32)
                scale = lax.rsqrt(jnp.mean(u * u, axis=1, keepdims=True) + eps)
                normed = acts[ui, wide, mine].astype(f32) * scale
                dbuf[rows, :] = d
                ps[rows, :] = jnp.broadcast_to(jnp.sum(d * normed, axis=1, keepdims=True), (32, 128))
                scb[rows, :] = jnp.broadcast_to(scale, (32, 128))

        tell = remote(ps, pr.at[b], p_send.at[b], p_recv.at[b], to_s)
        tell.start()
        tell.wait()

        @pl.loop(0, n // 32)
        def _(c):
            rows, wide = at(c * 32, 32), at(me * n + c * 32, 32)
            scale = scb[rows, 0:1]
            normed = acts[ui, wide, mine].astype(f32) * scale
            mean = (ps[rows, 0:1] + pr[b, rows, 0:1]) * (1.0 / D)
            d_u = acts[ci, wide, mine].astype(f32) + scale * (dbuf[rows, :] - normed * mean)
            store(rows, wide, d_u.astype(bf16))

    def product(k, side):
        cut = at(fs_of(k, side) * S, S, 128)
        return 0.5 * jnp.dot(hT[...], acts[3, :, cut], preferred_element_type=f32)

    def gy(k):
        return remote(gys.at[k], gyr.at[k], gy_send.at[k], gy_recv.at[k], to_y)

    def gfar(i):
        return remote(g2s.at[i], g2r.at[i], g2_send.at[i], g2_recv.at[i], to_z[2])

    def gnear(j):
        return remote(gzs, gq.at[j], gz_send.at[0], gz_recv.at[0], to_z[1])

    def gx(i, j):
        return remote(gq.at[j], gq.at[j], gx_send.at[i], gx_recv.at[i], to_x)

    def grad_y():
        for k in (3, 2, 1, 0):
            gys[k] = product(k, 1 - y).astype(bf16)
            gy(k).start()

    def grad_far():
        for i, k in enumerate((3, 2)):
            value = product(k, y)
            gy(k).wait_recv()
            g2s[i] = (value + gyr[k].astype(f32)).astype(bf16)
            gfar(i).start()

    def grad_near():
        value = product(1, y)
        gy(1).wait_recv()
        gfar(0).wait_recv()
        gzs[...] = (value + gyr[1].astype(f32) + g2r[0].astype(f32)).astype(bf16)
        gnear(me).start()
        value = product(0, y)
        gy(0).wait_recv()
        gfar(1).wait_recv()
        gq[me] = (value + gyr[0].astype(f32) + g2r[1].astype(f32)).astype(bf16)
        gx(0, me).start()

    def grad_x():
        gnear(jz).wait_recv()
        gx(1, jz).start()

    def tell(owner):
        return lambda k: remote(nb.at[owner], nb.at[owner], n_send.at[k - 1], n_recv.at[k - 1], {"fs": lax.rem(f + k, F)})

    def grad_out():
        gx(0, jx).wait_recv()
        gx(1, jd).wait_recv()
        for q in range(4):
            g = gq[q].astype(f32)
            grad[q * H : (q + 1) * H, :] = g
            square = g * g
            folded = square[:, 0:128]
            for lane in range(128, S, 128):
                folded = folded + square[:, lane : lane + 128]
            nb[f, :, q * H : (q + 1) * H] = jnp.sum(folded.T, axis=0, keepdims=True)
        for k in range(1, F):
            tell(f)(k).start()

    both, last = (0, 1), (2,)
    first, final = 2 - inn, 1 + inn

    def send(b, pieces, k, who):
        @pl.when(who)
        def _():
            for p in pieces:
                w_first(b, p, k).start()

    a_copy(0, 1).start()
    for p in (0, 1, 2):
        w_cross(1, p, 0).start()
    send(1, both, 1, outer)
    send(1, both, 2, inner)
    a_copy(0, 0).start()
    send(1, last, 1, outer)
    send(1, last, 2, inner)
    a_copy(1, 0).start()
    send(1, (0, 1, 2), 3, inner)
    send(1, (0, 1, 2), 2, outer)
    send(1, (0, 1, 2), 1, inner)

    serve(1, both, first, True)
    a_zn(0)
    a_copy(1, 1).start()
    serve(1, last, first, True)
    a_x(0)
    for c in loads.values():
        c.wait()
    serve(1, both, 3)
    a_d(0)
    a_s(0)
    normalise(0, 0, 2)
    serve(1, last, 3)
    normalise(0, 2, 4)
    forward(1, fs_of(0, y), True)
    crossed(1, both, 0)
    forward(1, fs_of(0, 1 - y))
    a_zn(1)
    send(0, (0, 1, 2), 3, inner)
    send(0, both, 1, outer)
    a_copy(2, 0).start()
    send(0, last, 1, outer)
    send(0, (0, 1, 2), 2, outer)
    send(0, (0, 1, 2), 2, inner)
    a_x(1)
    forward(1, fs_of(first, y))
    crossed(1, both, first)
    forward(1, fs_of(first, 1 - y))
    serve(1, both, final)
    forward(1, fs_of(3, y))
    crossed(1, both, 3)
    forward(1, fs_of(3, 1 - y))
    serve(1, last, final)
    a_copy(2, 1).start()
    for p in (0, 1, 2):
        w_cross(0, p, 0).start()
    a_d(1)
    forward(1, fs_of(final, y))
    a_s(1)
    for k in (0, first, 3):
        backed(1, 1, fs_of(k, y), isinstance(k, int) and k == 0)
        crossed(1, last, k)
        backed(1, 1, fs_of(k, 1 - y))
    backed(1, 1, fs_of(final, y))
    crossed(1, both, final)
    forward(1, fs_of(final, 1 - y))
    crossed(1, last, final)
    backed(1, 1, fs_of(final, 1 - y))
    elementwise()
    partials(1)
    x_step(1)
    serve(0, both, first, True)
    z_step(1, 0)
    z_step(1, 1)
    send(0, both, 1, inner)
    a_zn(2)
    serve(0, last, first, True)
    serve(0, both, 3)
    a_x(2)

    def to_mg(rows, wide, value):
        acts[3, wide, mine] = value

    finish(1, 0, 1, ((2, 0), (3, 1)), to_mg)
    for kind in (0, 1, 6):
        a_copy(3, kind).start()
    send(0, last, 1, inner)
    serve(0, last, 3)
    a_d(2)
    a_s(2)
    normalise(2, 0, 2)
    serve(0, both, final)
    a_zn(3)
    normalise(2, 2, 4)
    a_x(3)
    for k in (0, first, 3):
        forward(0, fs_of(k, y), isinstance(k, int) and k == 0)
        crossed(0, both, k)
        forward(0, fs_of(k, 1 - y))
    serve(0, last, final)
    forward(0, fs_of(final, y))
    crossed(0, both, final)
    forward(0, fs_of(final, 1 - y))
    hidden()
    a_d(3)
    a_s(3)
    grad_y()
    for k in (0, first, 3):
        backed(0, 3, fs_of(k, y), isinstance(k, int) and k == 0)
        crossed(0, last, k)
        backed(0, 3, fs_of(k, 1 - y))
    backed(0, 3, fs_of(final, y))
    for i, side in enumerate((1 - r, r)):
        sibling(1, i, side).wait_send()
    for piece in range(4):
        x_copy(1, piece).wait_send()
    for piece in range(2):
        z_copy(1, piece).wait_send()
    crossed(0, last, final)
    backed(0, 3, fs_of(final, 1 - y))
    elementwise()
    partials(0, spread)
    grad_far()
    spread_end()
    grad_near()

    def to_out(rows, wide, value):
        out[rows, mine] = value
        obs[rows, :] = value

    finish(0, 2, 3, ((1, 2), (2, 1)), to_out)
    swap = remote(obs, obr, o_send.at[0], o_recv.at[0], to_s)
    swap.start()
    grad_x()
    grad_out()
    swap.wait()
    out[:, other] = obr[...]

    for b in (1, 0):
        for p in range(3):
            for k in (1, 2):
                w_first(b, p, k).wait_send()
            for k in range(4):
                w_cross(b, p, k).wait_send()

            @pl.when(inner)
            def _(b=b, p=p):
                w_first(b, p, 3).wait_send()
                w_relay(b, p).wait_send()

    for i in range(4):
        for kind in range(7 if i == 3 else 6):
            a_copy(i, kind).wait_send()
    for i, side in enumerate((1 - r, r)):
        sibling(0, i, side).wait_send()
    for piece in range(3):
        x_copy(0, piece).wait_send()
        z_copy(0, piece).wait_send()
    for k in range(4):
        gy(k).wait_send()
    for i in range(2):
        gfar(i).wait_send()
    gnear(me).wait_send()
    gx(0, me).wait_send()
    gx(1, jz).wait_send()
    for k in range(1, F):
        tell(lax.rem(f + F - k, F))(k).wait_recv()
        tell(f)(k).wait_send()
    total = nb[0]
    for k in range(1, F):
        total = total + nb[k]
    norms[...] = total


def on_square(sizes, *arrays):
    R, F, T, n, D, H = sizes
    S, half, m = D // F, D // 2, 4 * n
    dma = pltpu.SemaphoreType.DMA
    vmem = pl.BlockSpec(memory_space=pltpu.VMEM)
    d_input, grad, norms = pl.pallas_call(
        functools.partial(square_kernel, sizes),
        out_shape=(
            jax.ShapeDtypeStruct((n, D), bf16),
            jax.ShapeDtypeStruct((4 * H, S), f32),
            jax.ShapeDtypeStruct((1, 4 * H), f32),
        ),
        in_specs=[pl.BlockSpec(memory_space=pl.ANY)] * 9,
        out_specs=(vmem, vmem, vmem),
        scratch_shapes=[
            pltpu.VMEM((2, D, 2 * H), bf16),
            pltpu.VMEM((2, H, D), bf16),
            pltpu.VMEM((4, m, D), bf16),
            pltpu.VMEM((m, D), bf16),
            pltpu.VMEM((m, 2 * H), f32),
            pltpu.VMEM((m, H), f32),
            pltpu.VMEM((m, 2 * H), bf16),
            pltpu.VMEM((H, m), bf16),
            pltpu.VMEM((m, D), bf16),
            pltpu.VMEM((2, m, half), bf16),
            pltpu.VMEM((2 * n, half), bf16),
            pltpu.VMEM((2, 2 * n, half), bf16),
            pltpu.VMEM((2 * n, half), bf16),
            pltpu.VMEM((2, 2 * n, half), bf16),
            pltpu.VMEM((n, half), f32),
            pltpu.VMEM((n, 128), f32),
            pltpu.VMEM((n, 128), f32),
            pltpu.VMEM((2, n, 128), f32),
            pltpu.VMEM((n, half), bf16),
            pltpu.VMEM((n, half), bf16),
            pltpu.VMEM((4, H, S), bf16),
            pltpu.VMEM((4, H, S), bf16),
            pltpu.VMEM((2, H, S), bf16),
            pltpu.VMEM((2, H, S), bf16),
            pltpu.VMEM((H, S), bf16),
            pltpu.VMEM((4, H, S), bf16),
            pltpu.VMEM((F, 1, 4 * H), f32),
            dma((9,)),
            dma((2, 3, 4)),
            dma((2, 3, 4)),
            dma((2, 3, 4)),
            dma((2, 3, 4)),
            dma((4, 7)),
            dma((4, 7)),
            dma((2, 2)),
            dma((2, 2)),
            dma((2, 4)),
            dma((2, 4)),
            dma((2, 4)),
            dma((2, 4)),
            dma((2,)),
            dma((2,)),
            dma((1,)),
            dma((1,)),
            dma((4,)),
            dma((4,)),
            dma((2,)),
            dma((2,)),
            dma((1,)),
            dma((1,)),
            dma((2,)),
            dma((2,)),
            dma((F - 1,)),
            dma((F - 1,)),
        ],
        compiler_params=pltpu.CompilerParams(
            collective_id=0, has_side_effects=True, vmem_limit_bytes=67043328
        ),
    )(*arrays)
    return d_input, grad, norms.reshape(-1)


def solution(mesh):
    R, F, T = (mesh.shape[a] for a in ("rep", "fs", "tp"))

    def whole(tokens, mid_tokens, out_grad, gate_first, *rest):
        D, FF = gate_first.shape
        n = tokens.shape[0] // (R * F)
        H = FF // (T * R)
        sizes = (R, F, T, n, D, H, 3 if F <= 8 and H % 384 == 0 else 1)
        body = functools.partial(on_device, sizes)
        if (R, F, T) == (2, 8, 2) and H % 256 == 0 and D % 1024 == 0 and n % 128 == 0:
            body = functools.partial(on_square, (R, F, T, n, D, H // 2))
        return jax.shard_map(
            body,
            mesh=mesh,
            in_specs=(P(("rep", "fs"), None),) * 3 + (P("fs", "tp"), P("fs", "tp"), P("tp", "fs")) * 2,
            out_specs=(P(("rep", "fs"), None), P("tp", "fs"), P("tp")),
            check_vma=False,
        )(tokens, mid_tokens, out_grad, gate_first, *rest)

    return whole
```

```python
import functools

import jax
import jax.numpy as jnp
from jax import lax
from jax.experimental import pallas as pl
from jax.experimental.pallas import tpu as pltpu
from jax.sharding import PartitionSpec as P

eps = 1e-06
f32, bf16 = jnp.float32, jnp.bfloat16


def kernel(sizes, tok, mid, cot, g1, u1, v1, g2, u2, v2, out, grad, norms, full1, downs1, full2, downs2, toks, mids, cots, mgs, xb, hidden, d_gate, d_up, mgt, gates, uppers, part, got1, snd2, got2, dn, rs_out, rs_in, gb, nb, w_send, w_recv, own_sem, x_send, x_recv, s1_send, s1_recv, s2_send, s2_recv, s3_send, s3_recv, r_send, r_recv, g_send, g_recv, n_send, n_recv):
    R, F, T, n, D, H, pieces = sizes
    S, half, C, width = D // F, D // F // 2, D // T, H // pieces
    both = 2 if pieces > 1 else 1
    r, f, t = (lax.axis_index(a) for a in ("rep", "fs", "tp"))

    def fs_at(position):
        q = lax.rem(position + 2 * F, F)
        hi = q // (F // 2)
        return (1 - hi) * 2 * q + hi * (2 * (F - 1 - q) + 1)

    odd = lax.rem(f, 2)
    p = (1 - odd) * (f // 2) + odd * (F - 1 - f // 2)
    side = (fs_at(p + 1), fs_at(p - 1))

    barrier = pltpu.get_barrier_semaphore()
    for axis, size, me in (("rep", R, r), ("fs", F, f), ("tp", T, t)):
        for k in range(1, size):
            pl.semaphore_signal(barrier, inc=1, device_id={axis: lax.rem(me + k, size)}, device_id_type=pl.DeviceIdType.MESH)
    pl.semaphore_wait(barrier, R + F + T - 3)

    def remote(src, dst, send, recv, **where):
        return pltpu.make_async_remote_copy(src_ref=src, dst_ref=dst, send_sem=send, recv_sem=recv, device_id=where, device_id_type=pl.DeviceIdType.MESH)

    fulls = ((full1, downs1), (full2, downs2))

    second_gu, second_d = (1, 0, both, 2 * H // both, 0), (1, 1, pieces, width, both)
    first_gu, first_d = (0,) + second_gu[1:], (0,) + second_d[1:]

    def ring(phase, d, distance, step, piece):
        b, which, count, wide, sem = phase
        owner = fs_at(p - distance if d == 0 else p + distance)
        rows = pl.ds(pl.multiple_of(owner * S + d * half, half), half)
        ref = fulls[b][which].at[rows]
        if count > 1:
            ref = fulls[b][which].at[rows, pl.ds(pl.multiple_of(piece * wide, 128), wide)]
        return remote(ref, ref, w_send.at[b, which, d], w_recv.at[b, d, step, sem + piece], fs=side[d])

    def start_ring(phase):
        for piece in range(phase[2]):
            for d in (0, 1):
                ring(phase, d, 0, 0, piece).start()

    def serve(phase, lo, hi, of):
        relays = (F - 2) * phase[2]

        @pl.loop(relays * lo // of, relays * hi // of)
        def _(k):
            step, piece = k // phase[2], lax.rem(k, phase[2])
            for d in (0, 1):
                ring(phase, d, step + 1, step, piece).wait_recv()
                ring(phase, d, step + 1, step + 1, piece).start()

    def end_ring(phase):
        for piece in range(phase[2]):
            for d in (0, 1):
                ring(phase, d, F - 1, F - 2, piece).wait_recv()

    def drain(b):
        for which in (0, 1):
            whole = fulls[b][which].at[pl.ds(0, (F - 1) * half)]
            for d in (0, 1):
                remote(whole, whole, w_send.at[b, which, d], w_recv.at[b, d, 0, 0], fs=side[d]).wait_send()

    mine = pl.ds(pl.multiple_of(r * n, n), n)
    pairs = (mids, cots, toks, mgs)
    held = pl.ds(pl.multiple_of(f * S, S), S)
    def pair_loads(g, u, full):
        if H % 128 > 0:
            return [(g, full.at[held])]
        taken = pl.ds(pl.multiple_of(r * H, 128), H)
        return [(g.at[:, taken], full.at[held, pl.ds(0, H)]), (u.at[:, taken], full.at[held, pl.ds(H, H)])]

    wanted = pair_loads(g2, u2, full2)
    ahead = len(wanted)
    wanted += [(mid, mids.at[mine]), (cot, cots.at[mine]), (tok, toks.at[mine]), (v2, downs2.at[held]), (v1, downs1.at[held])]
    wanted += pair_loads(g1, u1, full1)
    loads = [pltpu.make_async_copy(src, dst, own_sem.at[i]) for i, (src, dst) in enumerate(wanted)]
    for c in loads:
        c.start()

    def swap(i):
        return [remote(pairs[i].at[mine], pairs[i].at[mine], x_send.at[i, k - 1], x_recv.at[i, k - 1], rep=lax.rem(r + k, R)) for k in range(1, R)]

    def swap_in(i):
        for k in range(1, R):
            rows = pl.ds(pl.multiple_of(lax.rem(r + R - k, R) * n, n), n)
            remote(pairs[i].at[rows], pairs[i].at[rows], x_send.at[i, k - 1], x_recv.at[i, k - 1], rep=lax.rem(r + k, R)).wait_recv()

    for c in loads[:ahead]:
        c.wait()
    start_ring(second_gu)
    for i in range(3):
        loads[ahead + i].wait()
        for c in swap(i):
            c.start()
    for c in loads[ahead + 3 :]:
        c.wait()

    def normalise(pair):
        @pl.loop(0, R * n // 32)
        def _(i):
            rows = pl.ds(pl.multiple_of(i * 32, 32), 32)
            u = pair[rows, :].astype(f32)
            xb[rows, :] = (u * lax.rsqrt(jnp.mean(u * u, axis=1, keepdims=True) + eps)).astype(bf16)

    chunk = 256 if H % 256 == 0 else 128 if H % 128 == 0 else H

    def cols(which, j):
        if chunk == H:
            return pl.ds(which * H, H)
        return pl.ds(pl.multiple_of(which * H + j * chunk, 128), chunk)

    def forward(full):
        @pl.loop(0, H // chunk)
        def _(j):
            gate = jnp.dot(xb[...], full[:, cols(0, j)], preferred_element_type=f32)
            upper = jnp.dot(xb[...], full[:, cols(1, j)], preferred_element_type=f32)
            hidden[:, cols(0, j)] = (gate * jax.nn.sigmoid(gate) * upper).astype(bf16)
            gates[:, cols(0, j)] = gate
            uppers[:, cols(0, j)] = upper

    def backed(downs, c_ref):
        @pl.loop(0, H // chunk)
        def _(j):
            gate, upper = gates[:, cols(0, j)], uppers[:, cols(0, j)]
            back = 0.5 * jnp.dot(c_ref[...], downs[:, cols(0, j)], preferred_element_type=f32)
            logistic = jax.nn.sigmoid(gate)
            d_gate[:, cols(0, j)] = (back * upper * logistic * (1.0 + gate * (1.0 - logistic))).astype(bf16)
            d_up[:, cols(0, j)] = (back * gate * logistic).astype(bf16)

    dims = (((1,), (1,)), ((), ()))

    def backward(full, lo, hi):
        @pl.loop(lo, hi)
        def _(j):
            rows = pl.ds(pl.multiple_of(j * 256, 256), 256)
            total = lax.dot_general(d_gate[...], full[rows, 0:H], dims, preferred_element_type=f32)
            total = total + lax.dot_general(d_up[...], full[rows, H : 2 * H], dims, preferred_element_type=f32)
            part[:, rows] = total.astype(bf16)

    def block_of(k):
        return pl.ds(pl.multiple_of(k * C, 128), C)

    def stage1(b):
        return [remote(part.at[:, block_of(lax.rem(t + k, T))], got1.at[b, k - 1], s1_send.at[b, k - 1], s1_recv.at[b, k - 1], tp=lax.rem(t + k, T)) for k in range(1, T)]

    def stage2(b):
        return [remote(snd2.at[k - 1], got2.at[b, k - 1], s2_send.at[b, k - 1], s2_recv.at[b, k - 1], rep=lax.rem(r + k, R)) for k in range(1, R)]

    def stage3(b, owner):
        ref = dn.at[b, :, block_of(owner)]
        return lambda k: remote(ref, ref, s3_send.at[b, k - 1], s3_recv.at[b, k - 1], tp=lax.rem(t + k, T))

    def summed(b, base, i):
        rows = pl.ds(pl.multiple_of(base * n + i * 32, 32), 32)
        total = part[rows, block_of(t)].astype(f32)
        for k in range(T - 1):
            total = total + got1[b, k, rows, :].astype(f32)
        return total

    def reduce_tp(b):
        for c in stage1(b):
            c.wait()
        for k in range(1, R):
            @pl.loop(0, n // 32)
            def _(i, k=k):
                snd2[k - 1, pl.ds(pl.multiple_of(i * 32, 32), 32), :] = summed(b, lax.rem(r + k, R), i).astype(bf16)
        for c in stage2(b):
            c.start()

    def reduce_rep(b):
        for c in stage2(b):
            c.wait()

        @pl.loop(0, n // 32)
        def _(i):
            rows = pl.ds(pl.multiple_of(i * 32, 32), 32)
            total = summed(b, r, i)
            for k in range(R - 1):
                total = total + got2[b, k, rows, :].astype(f32)
            dn[b, rows, block_of(t)] = total.astype(bf16)

        for k in range(1, T):
            stage3(b, t)(k).start()

    def finish(b, pair, carried, result, offset):
        for k in range(1, T):
            stage3(b, lax.rem(t + T - k, T))(k).wait_recv()
            stage3(b, t)(k).wait_send()

        @pl.loop(0, n // 32)
        def _(i):
            rows = pl.ds(pl.multiple_of(i * 32, 32), 32)
            wide = pl.ds(pl.multiple_of(r * n + i * 32, 32), 32)
            u = pair[wide, :].astype(f32)
            scale = lax.rsqrt(jnp.mean(u * u, axis=1, keepdims=True) + eps)
            normed = u * scale
            d = dn[b, rows, :].astype(f32)
            d_u = carried[wide, :].astype(f32) + scale * (d - normed * jnp.mean(d * normed, axis=1, keepdims=True))
            result[pl.ds(pl.multiple_of(offset + i * 32, 32), 32), :] = d_u.astype(bf16)

    serve(second_gu, 0, 10, 12)
    swap_in(0)
    normalise(mids)
    serve(second_gu, 10, 12, 12)
    start_ring(second_d)
    end_ring(second_gu)
    serve(second_d, 0, 3, 18)
    forward(full2)
    serve(second_d, 3, 18, 18)
    start_ring(first_gu)
    swap_in(1)
    end_ring(second_d)
    backed(downs2, cots)
    serve(first_gu, 0, 1, 12)
    backward(full2, 0, D // 512)
    serve(first_gu, 1, 2, 12)
    backward(full2, D // 512, D // 256)
    for c in stage1(1):
        c.start()
    serve(first_gu, 2, 3, 12)
    reduce_tp(1)
    serve(first_gu, 3, 4, 12)
    swap_in(2)
    normalise(toks)
    serve(first_gu, 4, 6, 12)
    reduce_rep(1)
    serve(first_gu, 6, 7, 12)
    finish(1, mids, cots, mgs, r * n)
    for c in swap(3):
        c.start()
    serve(first_gu, 7, 12, 12)
    start_ring(first_d)
    end_ring(first_gu)

    forward(full1)
    serve(first_d, 0, 6, 18)
    swap_in(3)

    @pl.loop(0, D // 256)
    def _(j):
        part_cols = pl.ds(pl.multiple_of(j * 256, 256), 256)
        mgt[part_cols, :] = mgs[:, part_cols].T

    serve(first_d, 6, 18, 18)

    def strip(piece):
        return pl.ds(pl.multiple_of(piece * width, 128), width) if pieces > 1 else slice(None)

    def product(d, position, piece):
        rows = pl.ds(pl.multiple_of(fs_at(position) * S + d * half, half), half)
        return 0.5 * jnp.dot(mgt[rows, :], hidden[:, strip(piece)], preferred_element_type=f32)

    def view(ref, piece):
        return ref.at[:, strip(piece)] if pieces > 1 else ref

    def rs(d, s, piece):
        return remote(view(rs_out.at[d, s], piece), view(rs_in.at[d, s], piece), r_send.at[d, s, piece], r_recv.at[d, s, piece], fs=side[d])

    def passed(lo, hi):
        @pl.loop(1 + (F - 2) * lo // 6, 1 + (F - 2) * hi // 6)
        def _(s):
            for piece in range(pieces):
                for d in (0, 1):
                    value = product(d, p - 1 - s if d == 0 else p + 1 + s, piece)
                    rs(d, s - 1, piece).wait_recv()
                    rs_out[d, s, :, strip(piece)] = (value + rs_in[d, s - 1, :, strip(piece)].astype(f32)).astype(bf16)
                    rs(d, s, piece).start()

    for piece in range(pieces):
        for d in (0, 1):
            rs_out[d, 0, :, strip(piece)] = product(d, p - 1 if d == 0 else p + 1, piece).astype(bf16)
            rs(d, 0, piece).start()
    end_ring(first_d)
    backed(downs1, mgs)
    passed(0, 1)
    backward(full1, 0, D // 512)
    passed(1, 2)
    backward(full1, D // 512, D // 256)
    for c in stage1(0):
        c.start()
    passed(2, 3)
    reduce_tp(0)
    passed(3, 6)

    def trade(owner, piece):
        ref = view(gb.at[owner], piece)
        return lambda k: remote(ref, ref, g_send.at[k - 1, piece], g_recv.at[k - 1, piece], rep=lax.rem(r + k, R))

    for piece in range(pieces):
        for d in (0, 1):
            value = product(d, p, piece)
            rs(d, F - 2, piece).wait_recv()
            gb[r, pl.ds(d * half, half), strip(piece)] = (value + rs_in[d, F - 2, :, strip(piece)].astype(f32)).astype(bf16)
        for k in range(1, R):
            trade(r, piece)(k).start()
    reduce_rep(0)
    finish(0, toks, mgs, out, 0)
    for piece in range(pieces):
        for k in range(1, R):
            trade(lax.rem(r + R - k, R), piece)(k).wait_recv()
            trade(r, piece)(k).wait_send()
    for k in range(R):
        g = gb[k].astype(f32)
        grad[:, k * H : (k + 1) * H] = g
        nb[f, :, k * H : (k + 1) * H] = jnp.sum(g * g, axis=0, keepdims=True)

    def tell(owner):
        return lambda k: remote(nb.at[owner], nb.at[owner], n_send.at[k - 1], n_recv.at[k - 1], fs=lax.rem(f + k, F))

    for k in range(1, F):
        tell(f)(k).start()
    for b in (0, 1):
        drain(b)
    for i in range(4):
        for c in swap(i):
            c.wait_send()

    @pl.loop(0, F - 1)
    def _(s):
        for piece in range(pieces):
            for d in (0, 1):
                rs(d, s, piece).wait_send()

    for k in range(1, F):
        tell(lax.rem(f + F - k, F))(k).wait_recv()
        tell(f)(k).wait_send()
    total = nb[0]
    for k in range(1, F):
        total = total + nb[k]
    norms[...] = total


def on_device(sizes, tokens, mid_tokens, out_grad, gate_first, up_first, down_first, gate_second, up_second, down_second):
    R, F, T, n, D, H, pieces = sizes
    S, half = D // F, D // F // 2
    start = lax.axis_index("rep") * H

    def own(gate_w, up_w, down_w):
        down = lax.dynamic_slice_in_dim(down_w, start, H, 0).T
        if H % 128 == 0:
            return gate_w, up_w, down
        pair = [lax.dynamic_slice_in_dim(w, start, H, 1) for w in (gate_w, up_w)]
        return jnp.concatenate(pair, axis=1), up_w, down

    dma = pltpu.SemaphoreType.DMA
    m = R * n
    any_space = pl.BlockSpec(memory_space=pl.ANY)
    vmem = pl.BlockSpec(memory_space=pltpu.VMEM)
    d_input, grad, norms = pl.pallas_call(
        functools.partial(kernel, sizes),
        out_shape=(
            jax.ShapeDtypeStruct((n, D), bf16),
            jax.ShapeDtypeStruct((S, R * H), f32),
            jax.ShapeDtypeStruct((1, R * H), f32),
        ),
        in_specs=[any_space] * 9,
        out_specs=(vmem, vmem, vmem),
        scratch_shapes=[
            pltpu.VMEM((D, 2 * H), bf16),
            pltpu.VMEM((D, H), bf16),
            pltpu.VMEM((D, 2 * H), bf16),
            pltpu.VMEM((D, H), bf16),
            pltpu.VMEM((m, D), bf16),
            pltpu.VMEM((m, D), bf16),
            pltpu.VMEM((m, D), bf16),
            pltpu.VMEM((m, D), bf16),
            pltpu.VMEM((m, D), bf16),
            pltpu.VMEM((m, H), bf16),
            pltpu.VMEM((m, H), bf16),
            pltpu.VMEM((m, H), bf16),
            pltpu.VMEM((D, m), bf16),
            pltpu.VMEM((m, H), f32),
            pltpu.VMEM((m, H), f32),
            pltpu.VMEM((m, D), bf16),
            pltpu.VMEM((2, T - 1, m, D // T), bf16),
            pltpu.VMEM((R - 1, n, D // T), bf16),
            pltpu.VMEM((2, R - 1, n, D // T), bf16),
            pltpu.VMEM((2, n, D), bf16),
            pltpu.VMEM((2, F - 1, half, H), bf16),
            pltpu.VMEM((2, F - 1, half, H), bf16),
            pltpu.VMEM((R, S, H), bf16),
            pltpu.VMEM((F, 1, R * H), f32),
            dma((2, 2, 2)),
            dma((2, 2, F - 1, pieces + (2 if pieces > 1 else 1))),
            dma((9,)),
            dma((4, R - 1)),
            dma((4, R - 1)),
            dma((2, T - 1)),
            dma((2, T - 1)),
            dma((2, R - 1)),
            dma((2, R - 1)),
            dma((2, T - 1)),
            dma((2, T - 1)),
            dma((2, F - 1, pieces)),
            dma((2, F - 1, pieces)),
            dma((R - 1, pieces)),
            dma((R - 1, pieces)),
            dma((F - 1,)),
            dma((F - 1,)),
        ],
        compiler_params=pltpu.CompilerParams(
            collective_id=0, has_side_effects=True, vmem_limit_bytes=67043328
        ),
    )(
        tokens,
        mid_tokens,
        out_grad,
        *own(gate_first, up_first, down_first),
        *own(gate_second, up_second, down_second),
    )
    return d_input, grad.T, norms.reshape(-1)


def square_kernel(sizes, tok, mid, cot, g1, u1, v1, g2, u2, v2, out, grad, norms, gu, dd, acts, xb, acc, bk, dg, hT, part, sib, xs, xr, zs, zr, dbuf, scb, ps, pr, obs, obr, gys, gyr, g2s, g2r, gzs, gq, nb, own_sem, wz_send, wz_recv, wy_send, wy_recv, a_send, a_recv, s_send, s_recv, x_send, x_recv, z_send, z_recv, p_send, p_recv, o_send, o_recv, gy_send, gy_recv, g2_send, g2_recv, gz_send, gz_recv, gx_send, gx_recv, n_send, n_recv):
    R, F, T, n, D, H = sizes
    S, half, h = D // F, D // 2, n // 2
    r, f, t = (lax.axis_index(a) for a in ("rep", "fs", "tp"))
    z, y = f // 2, lax.rem(f, 2)
    zl, zh = lax.rem(z, 2), z // 2

    def fs_of(k, side):
        return 2 * (2 * lax.rem(zh + k // 2, 2) + lax.rem(zl + k % 2, 2)) + side

    to_x, to_y, to_s = {"rep": 1 - r}, {"fs": fs_of(0, 1 - y)}, {"tp": 1 - t}
    to_z = [None] + [{"fs": fs_of(k, y)} for k in (1, 2, 3)]
    inn = lax.rem(zl + zh, 2)
    inner, outer = inn == 1, inn == 0
    me, jx, jz, jd = 2 * r + zl, 2 * (1 - r) + zl, 2 * r + 1 - zl, 2 * (1 - r) + 1 - zl

    barrier = pltpu.get_barrier_semaphore()
    for axis, size, at in (("rep", R, r), ("fs", F, f), ("tp", T, t)):
        for k in range(1, size):
            pl.semaphore_signal(barrier, inc=1, device_id={axis: lax.rem(at + k, size)}, device_id_type=pl.DeviceIdType.MESH)

    def at(start, size, step=8):
        return pl.ds(pl.multiple_of(start, step), size)

    def remote(src, dst, send, recv, where):
        return pltpu.make_async_remote_copy(src_ref=src, dst_ref=dst, send_sem=send, recv_sem=recv, device_id=where, device_id_type=pl.DeviceIdType.MESH)

    weights = ((g1, u1, v1), (g2, u2, v2))
    fields = (mid, cot, tok)

    def source(b, p, q):
        ref = weights[b][p]
        return ref.at[at(q * H, H)] if p == 2 else ref.at[:, at(q * H, H, 128)]

    def place(b, p, owner):
        if p == 2:
            return dd.at[b, :, at(owner * S, S, 128)]
        return gu.at[b, at(owner * S, S), pl.ds(p * H, H)]

    loads = {}
    for i in range(3):
        loads["a", i] = pltpu.make_async_copy(fields[i], acts.at[i, at(me * n, n)], own_sem.at[i])
    for b in (1, 0):
        for p in range(3):
            loads["w", b, p] = pltpu.make_async_copy(source(b, p, me), place(b, p, f), own_sem.at[3 + 3 * b + p])
    for c in loads.values():
        c.start()
    pl.semaphore_wait(barrier, R + F + T - 3)

    def w_first(b, p, k):
        q = me if k == 2 else jz
        return remote(source(b, p, q), place(b, p, f), wz_send.at[b, p, k], wz_recv.at[b, p, k], to_z[k])

    def w_relay(b, p):
        ref = place(b, p, fs_of(1, y))
        return remote(ref, ref, wz_send.at[b, p, 0], wz_recv.at[b, p, 3], to_z[2])

    def w_cross(b, p, k):
        ref = place(b, p, fs_of(k, y))
        return remote(source(b, p, me) if isinstance(k, int) and k == 0 else ref, ref, wy_send.at[b, p, k], wy_recv.at[b, p, k], to_y)

    def w_arrived(b, p, k):
        ref = place(b, p, fs_of(k, y))
        remote(ref, ref, wz_send.at[b, p, k], wz_recv.at[b, p, k], to_z[1]).wait_recv()

    def crossed(b, pieces, k):
        for p in pieces:
            ref = place(b, p, fs_of(k, 1 - y))
            remote(ref, ref, wy_send.at[b, p, k], wy_recv.at[b, p, k], to_y).wait_recv()

    def serve(b, pieces, k, near=False):
        for p in pieces:
            w_arrived(b, p, k)
            if near:
                @pl.when(inner)
                def _(p=p):
                    w_relay(b, p).start()
            w_cross(b, p, k).start()

    mine, other = at(t * half, half, 128), at((1 - t) * half, half, 128)

    def rows_of(j):
        return at(j * n, n)

    def a_copy(i, kind):
        if kind < 2:
            dst = acts.at[i, rows_of(me), mine]
            return remote(fields[i].at[:, mine] if i < 3 else dst, dst, a_send.at[i, kind], a_recv.at[i, kind], (to_z[1], to_x)[kind])
        ref = acts.at[i, rows_of({2: jz, 3: jz, 4: jx, 5: jd, 6: me}[kind]), mine]
        return remote(ref, ref, a_send.at[i, kind], a_recv.at[i, kind], to_x if kind == 2 else to_s)

    def a_arrived(i, kind):
        j = (jz, jx, jd, jz, jx, jd, me)[kind]
        ref = acts.at[i, rows_of(j), mine if kind < 3 else other]
        remote(ref, ref, a_send.at[i, kind], a_recv.at[i, kind], to_x).wait_recv()

    def a_zn(i):
        a_arrived(i, 0)
        a_copy(i, 2).start()
        a_copy(i, 3).start()

    def a_x(i):
        a_arrived(i, 1)
        a_copy(i, 4).start()

    def a_d(i):
        a_arrived(i, 2)
        a_copy(i, 5).start()

    def a_s(i):
        for kind in (3, 4, 5) + ((6,) if i == 3 else ()):
            a_arrived(i, kind)

    def normalise(i, lo, hi):
        @pl.loop(lo * n // 32, hi * n // 32)
        def _(c):
            rows = at(c * 32, 32)
            u = acts[i, rows, :].astype(f32)
            xb[rows, :] = (u * lax.rsqrt(jnp.mean(u * u, axis=1, keepdims=True) + eps)).astype(bf16)

    nt = (((1,), (1,)), ((), ()))

    def forward(b, owner, first=False):
        cut = at(owner * S, S, 128)

        @pl.loop(0, 2 * H // 256)
        def _(j):
            cols = at(j * 256, 256, 128)
            value = jnp.dot(xb[:, cut], gu[b, at(owner * S, S), cols], preferred_element_type=f32)
            acc[:, cols] = value if first else acc[:, cols] + value

    def backed(b, i, owner, blocks, fresh=False):
        cut = at(owner * S, S, 128)

        def update(rows):
            value = lax.dot_general(acts[i, rows, cut], dd[b, :, cut], nt, preferred_element_type=f32)
            bk[rows, :] = value if fresh else bk[rows, :] + value

        if blocks == 4:
            @pl.loop(0, 2)
            def _(c):
                update(at(c * 2 * n, 2 * n))
        elif blocks == 3:
            @pl.loop(1, 4)
            def _(c):
                update(rows_of(lax.rem(jd + c, 4)))
        else:
            update(rows_of(jd))

    def hidden():
        @pl.loop(0, 4 * n // 128)
        def _(c):
            rows = at(c * 128, 128)
            gate = acc[rows, 0:H]
            hT[:, at(c * 128, 128, 128)] = (gate * jax.nn.sigmoid(gate) * acc[rows, H : 2 * H]).astype(bf16).T

    def elementwise(lo, hi):
        @pl.loop(lo * n // 64, hi * n // 64)
        def _(c):
            block = lax.rem(jd + c // (n // 64), 4)
            rows = at(block * n + lax.rem(c, n // 64) * 64, 64)
            gate, upper, back = acc[rows, 0:H], acc[rows, H : 2 * H], 0.5 * bk[rows, :]
            logistic = jax.nn.sigmoid(gate)
            dg[rows, 0:H] = (back * upper * logistic * (1.0 + gate * (1.0 - logistic))).astype(bf16)
            dg[rows, H : 2 * H] = (back * gate * logistic).astype(bf16)

    def partial(b, rows, c):
        @pl.loop(0, half // 256)
        def _(j):
            wide = c * half + j * 256
            total = lax.dot_general(dg[rows, :], gu[b, at(wide, 256), :], nt, preferred_element_type=f32)
            part[rows, at(wide, 256, 128)] = total.astype(bf16)

    def group(i):
        return (rows_of(jd), rows_of(jx), at(r * 2 * n, 2 * n))[i]

    def sibling(b, i):
        return remote(part.at[group(i), other], sib.at[b, group(i)], s_send.at[b, i], s_recv.at[b, i], to_s)

    def partials(b, i):
        partial(b, group(i), 1 - t)
        sibling(b, i).start()
        partial(b, group(i), t)

    def x_copy(b, piece):
        rows = pl.ds(piece * h, h)
        return remote(xs.at[rows], xr.at[b, rows], x_send.at[b, piece], x_recv.at[b, piece], to_x)

    def z_copy(b, piece):
        rows = pl.ds(piece * h, h)
        return remote(zs.at[rows], zr.at[b, rows], z_send.at[b, piece], z_recv.at[b, piece], to_z[1])

    def own_sum(b, rows):
        return part[rows, mine].astype(f32) + sib[b, rows, :].astype(f32)

    def x_step(b, lo, hi):
        for piece in range(lo, hi):
            base = (jd if piece < 2 else jx) * n + (piece % 2) * h
            sum_send(b, xs, piece, base, None, x_copy)

    def z_step(b, piece):
        x_copy(b, piece).wait_recv()

        @pl.loop(0, h // 32)
        def _(c):
            rows = at(piece * h + c * 32, 32)
            total = own_sum(b, at(jz * n + piece * h + c * 32, 32)) + xr[b, rows, :].astype(f32)
            zs[rows, :] = total.astype(bf16)

        z_copy(b, piece).start()

    def sum_send(b, buf, piece, base, extra, copy):
        @pl.loop(0, h // 32)
        def _(c):
            total = own_sum(b, at(base + c * 32, 32))
            if extra is not None:
                total = total + extra[b, at(c * 32, 32), :].astype(f32)
            buf[at(piece * h + c * 32, 32), :] = total.astype(bf16)

        copy(b, piece).start()

    def spread_x():
        z_copy(0, 0).wait_recv()
        sum_send(0, xs, 2, jx * n + h, zr, x_copy)

    def spread_z():
        x_copy(0, 0).wait_recv()
        sum_send(0, zs, 2, jz * n, xr, z_copy)

    def finish(b, ui, ci, parts, store, done):
        for piece, px, pz in parts:
            x_copy(b, px).wait_recv()
            z_copy(b, pz).wait_recv()

            @pl.loop(piece * h // 32, (piece + 1) * h // 32)
            def _(c, piece=piece, px=px, pz=pz):
                rows, wide = at(c * 32, 32), at(me * n + c * 32, 32)
                from_x, from_z = (at((q - piece) * h + c * 32, 32) for q in (px, pz))
                d = own_sum(b, wide) + xr[b, from_x, :].astype(f32) + zr[b, from_z, :].astype(f32)
                u = acts[ui, wide, :].astype(f32)
                scale = lax.rsqrt(jnp.mean(u * u, axis=1, keepdims=True) + eps)
                normed = acts[ui, wide, mine].astype(f32) * scale
                dbuf[rows, :] = d
                ps[rows, :] = jnp.broadcast_to(jnp.sum(d * normed, axis=1, keepdims=True), (32, 128))
                scb[rows, :] = jnp.broadcast_to(scale, (32, 128))

            part_rows = pl.ds(piece * h, h)
            tell_half = remote(ps.at[part_rows], pr.at[b, part_rows], p_send.at[b, piece], p_recv.at[b, piece], to_s)
            tell_half.start()
            tell_half.wait()

            @pl.loop(piece * h // 32, (piece + 1) * h // 32)
            def _(c):
                rows, wide = at(c * 32, 32), at(me * n + c * 32, 32)
                scale = scb[rows, 0:1]
                normed = acts[ui, wide, mine].astype(f32) * scale
                mean = (ps[rows, 0:1] + pr[b, rows, 0:1]) * (1.0 / D)
                d_u = acts[ci, wide, mine].astype(f32) + scale * (dbuf[rows, :] - normed * mean)
                store(rows, wide, d_u.astype(bf16))

            done(piece)

    def product(k, side):
        cut = at(fs_of(k, side) * S, S, 128)
        return 0.5 * jnp.dot(hT[...], acts[3, :, cut], preferred_element_type=f32)

    def gy(k):
        return remote(gys.at[k], gyr.at[k], gy_send.at[k], gy_recv.at[k], to_y)

    def gfar(i):
        return remote(g2s.at[i], g2r.at[i], g2_send.at[i], g2_recv.at[i], to_z[2])

    def gnear(j):
        return remote(gzs, gq.at[j], gz_send.at[0], gz_recv.at[0], to_z[1])

    def gx(i, j):
        return remote(gq.at[j], gq.at[j], gx_send.at[i], gx_recv.at[i], to_x)

    def grad_y(k):
        gys[k] = product(k, 1 - y).astype(bf16)
        gy(k).start()

    def grad_far(i, k):
        value = product(k, y)
        gy(k).wait_recv()
        g2s[i] = (value + gyr[k].astype(f32)).astype(bf16)
        gfar(i).start()

    def grad_near():
        value = product(1, y)
        gy(1).wait_recv()
        gfar(0).wait_recv()
        gzs[...] = (value + gyr[1].astype(f32) + g2r[0].astype(f32)).astype(bf16)
        gnear(me).start()

    def grad_own():
        value = product(0, y)
        gy(0).wait_recv()
        gfar(1).wait_recv()
        gq[me] = (value + gyr[0].astype(f32) + g2r[1].astype(f32)).astype(bf16)
        gx(0, me).start()

    def grad_x():
        gnear(jz).wait_recv()
        gx(1, jz).start()

    def tell(owner):
        return lambda k: remote(nb.at[owner], nb.at[owner], n_send.at[k - 1], n_recv.at[k - 1], {"fs": lax.rem(f + k, F)})

    def grad_out():
        gx(0, jx).wait_recv()
        gx(1, jd).wait_recv()
        for q in range(4):
            g = gq[q].astype(f32)
            grad[q * H : (q + 1) * H, :] = gq[q]
            square = g * g
            folded = square[:, 0:128]
            for lane in range(128, S, 128):
                folded = folded + square[:, lane : lane + 128]
            row = jnp.sum(folded.T, axis=0, keepdims=True)
            for c in range(H // 128):
                nb[f, q * H // 128 + c, :] = row[0, c * 128 : (c + 1) * 128]
        for k in range(1, F):
            tell(f)(k).start()

    both, last, every = (0, 1), (2,), (0, 1, 2)
    first, final = 2 - inn, 1 + inn

    def send(b, pieces, k, who):
        @pl.when(who)
        def _():
            for p in pieces:
                w_first(b, p, k).start()

    a_copy(0, 1).start()
    for p in every:
        w_cross(1, p, 0).start()
    send(1, every, 3, inner)
    send(1, every, 2, inner)
    send(1, both, 1, outer)
    a_copy(0, 0).start()
    send(1, last, 1, outer)
    a_copy(1, 0).start()
    send(1, every, 1, inner)
    send(1, every, 2, outer)

    a_zn(0)
    a_copy(1, 1).start()
    serve(1, both, first, True)
    a_x(0)
    a_d(0)
    for c in loads.values():
        c.wait()
    a_s(0)
    normalise(0, 0, 4)
    forward(1, fs_of(0, y), True)
    serve(1, last, first, True)
    send(0, every, 3, inner)
    send(0, both, 2, inner)
    send(0, both, 1, outer)
    a_copy(2, 0).start()
    send(0, last, 1, outer)
    send(0, every, 2, outer)
    serve(1, (0,), 3)
    a_zn(1)
    a_copy(2, 1).start()
    serve(1, (1,), 3)
    crossed(1, both, 0)
    forward(1, fs_of(0, 1 - y))
    a_x(1)
    forward(1, fs_of(first, y))
    crossed(1, both, first)
    forward(1, fs_of(first, 1 - y))
    serve(1, both, final)
    forward(1, fs_of(3, y))
    serve(1, last, 3)
    serve(1, last, final)
    for p in every:
        w_cross(0, p, 0).start()
    a_d(1)
    crossed(1, both, 3)
    forward(1, fs_of(3, 1 - y))
    forward(1, fs_of(final, y))
    a_s(1)
    backed(1, 1, fs_of(0, y), 4, True)
    crossed(1, last, 0)
    backed(1, 1, fs_of(0, 1 - y), 4)
    backed(1, 1, fs_of(first, y), 4)
    crossed(1, last, first)
    backed(1, 1, fs_of(first, 1 - y), 4)
    backed(1, 1, fs_of(3, y), 4)
    backed(1, 1, fs_of(final, y), 4)
    crossed(1, both, final)
    forward(1, fs_of(final, 1 - y))
    crossed(1, last, 3)
    backed(1, 1, fs_of(3, 1 - y), 4)
    crossed(1, last, final)
    backed(1, 1, fs_of(final, 1 - y), 4)
    elementwise(0, 1)
    partials(1, 0)
    elementwise(1, 4)
    sibling(1, 0).wait_recv()
    x_step(1, 0, 2)
    partials(1, 1)
    sibling(1, 1).wait_recv()
    x_step(1, 2, 4)
    partials(1, 2)
    sibling(1, 2).wait_recv()
    z_step(1, 0)
    a_zn(2)
    z_step(1, 1)
    send(0, last, 2, inner)
    serve(0, every, first, True)
    a_x(2)

    def to_mg(rows, wide, value):
        acts[3, wide, mine] = value

    finish(1, 0, 1, ((0, 2, 0), (1, 3, 1)), to_mg, lambda piece: None)
    for kind in (1, 0, 6):
        a_copy(3, kind).start()
    send(0, every, 1, inner)
    serve(0, every, 3)

    @pl.when(inner)
    def _():
        serve(0, every, 2)

    a_d(2)
    a_s(2)
    normalise(2, 0, 4)
    a_zn(3)
    for k in (0, first):
        forward(0, fs_of(k, y), isinstance(k, int))
        crossed(0, both, k)
        forward(0, fs_of(k, 1 - y))
    @pl.when(outer)
    def _():
        serve(0, (0,), 1)

    a_x(3)
    forward(0, fs_of(3, y))
    crossed(0, both, 3)
    forward(0, fs_of(3, 1 - y))
    @pl.when(outer)
    def _():
        serve(0, (1,), 1)

    for kind in (6, 3, 4):
        a_arrived(3, kind)
    for k in (0, first):
        backed(0, 3, fs_of(k, y), 3, isinstance(k, int))
        crossed(0, last, k)
        backed(0, 3, fs_of(k, 1 - y), 3)
    @pl.when(outer)
    def _():
        serve(0, last, 1)

    backed(0, 3, fs_of(3, y), 3)
    crossed(0, last, 3)
    backed(0, 3, fs_of(3, 1 - y), 3)
    forward(0, fs_of(final, y))
    crossed(0, both, final)
    forward(0, fs_of(final, 1 - y))
    hidden()
    a_d(3)
    for i in range(3):
        sibling(1, i).wait_send()
    for piece in range(4):
        x_copy(1, piece).wait_send()
    for piece in range(2):
        z_copy(1, piece).wait_send()
    a_arrived(3, 5)
    grad_y(3)
    for k in (0, first, 3):
        for side in (y, 1 - y):
            backed(0, 3, fs_of(k, side), 1, isinstance(k, int) and k == 0 and side is y)
    backed(0, 3, fs_of(final, y), 1)
    crossed(0, last, final)
    backed(0, 3, fs_of(final, 1 - y), 1)
    elementwise(0, 1)
    partials(0, 0)
    grad_y(2)
    sibling(0, 0).wait_recv()
    sum_send(0, xs, 0, jd * n, None, x_copy)
    sum_send(0, zs, 0, jd * n + h, None, z_copy)
    grad_far(0, 3)
    grad_y(1)
    backed(0, 3, fs_of(final, y), 3)
    backed(0, 3, fs_of(final, 1 - y), 3)
    elementwise(1, 4)
    partials(0, 1)
    grad_far(1, 2)
    sibling(0, 1).wait_recv()
    sum_send(0, xs, 1, jx * n, None, x_copy)
    grad_y(0)
    partials(0, 2)
    spread_x()
    grad_near()
    sibling(0, 2).wait_recv()
    sum_send(0, zs, 1, jz * n + h, None, z_copy)
    spread_z()
    grad_own()
    grad_x()

    def to_out(rows, wide, value):
        out[rows, mine] = value
        obs[rows, :] = value

    def swap(piece):
        rows = pl.ds(piece * h, h)
        return remote(obs.at[rows], obr.at[rows], o_send.at[piece], o_recv.at[piece], to_s)

    def half_done(piece):
        swap(piece).start()
        if piece == 1:
            grad_out()

    finish(0, 2, 3, ((1, 2, 1), (0, 1, 2)), to_out, half_done)
    for piece in (1, 0):
        swap(piece).wait()
    out[:, other] = obr[...]

    for b in (1, 0):
        for p in range(3):
            for k in (1, 2):
                w_first(b, p, k).wait_send()
            for k in range(4):
                w_cross(b, p, k).wait_send()

            @pl.when(inner)
            def _(b=b, p=p):
                w_first(b, p, 3).wait_send()
                w_relay(b, p).wait_send()

    for i in range(4):
        for kind in range(7 if i == 3 else 6):
            a_copy(i, kind).wait_send()
    for i in range(3):
        sibling(0, i).wait_send()
    for piece in range(3):
        x_copy(0, piece).wait_send()
        z_copy(0, piece).wait_send()
    for k in range(4):
        gy(k).wait_send()
    for i in range(2):
        gfar(i).wait_send()
    gnear(me).wait_send()
    gx(0, me).wait_send()
    gx(1, jz).wait_send()
    for k in range(1, F):
        tell(lax.rem(f + F - k, F))(k).wait_recv()
        tell(f)(k).wait_send()
    total = nb[0]
    for k in range(1, F):
        total = total + nb[k]
    norms[...] = total


def on_square(sizes, *arrays):
    R, F, T, n, D, H = sizes
    S, half, m = D // F, D // 2, 4 * n
    dma = pltpu.SemaphoreType.DMA
    vmem = pl.BlockSpec(memory_space=pltpu.VMEM)
    d_input, grad, norms = pl.pallas_call(
        functools.partial(square_kernel, sizes),
        out_shape=(
            jax.ShapeDtypeStruct((n, D), bf16),
            jax.ShapeDtypeStruct((4 * H, S), bf16),
            jax.ShapeDtypeStruct((4 * H // 128, 128), f32),
        ),
        in_specs=[pl.BlockSpec(memory_space=pl.ANY)] * 9,
        out_specs=(vmem, vmem, vmem),
        scratch_shapes=[
            pltpu.VMEM((2, D, 2 * H), bf16),
            pltpu.VMEM((2, H, D), bf16),
            pltpu.VMEM((4, m, D), bf16),
            pltpu.VMEM((m, D), bf16),
            pltpu.VMEM((m, 2 * H), f32),
            pltpu.VMEM((m, H), f32),
            pltpu.VMEM((m, 2 * H), bf16),
            pltpu.VMEM((H, m), bf16),
            pltpu.VMEM((m, D), bf16),
            pltpu.VMEM((2, m, half), bf16),
            pltpu.VMEM((2 * n, half), bf16),
            pltpu.VMEM((2, 2 * n, half), bf16),
            pltpu.VMEM((2 * n, half), bf16),
            pltpu.VMEM((2, 2 * n, half), bf16),
            pltpu.VMEM((n, half), f32),
            pltpu.VMEM((n, 128), f32),
            pltpu.VMEM((n, 128), f32),
            pltpu.VMEM((2, n, 128), f32),
            pltpu.VMEM((n, half), bf16),
            pltpu.VMEM((n, half), bf16),
            pltpu.VMEM((4, H, S), bf16),
            pltpu.VMEM((4, H, S), bf16),
            pltpu.VMEM((2, H, S), bf16),
            pltpu.VMEM((2, H, S), bf16),
            pltpu.VMEM((H, S), bf16),
            pltpu.VMEM((4, H, S), bf16),
            pltpu.VMEM((F, 4 * H // 128, 128), f32),
            dma((9,)),
            dma((2, 3, 4)),
            dma((2, 3, 4)),
            dma((2, 3, 4)),
            dma((2, 3, 4)),
            dma((4, 7)),
            dma((4, 7)),
            dma((2, 3)),
            dma((2, 3)),
            dma((2, 4)),
            dma((2, 4)),
            dma((2, 4)),
            dma((2, 4)),
            dma((2, 2)),
            dma((2, 2)),
            dma((2,)),
            dma((2,)),
            dma((4,)),
            dma((4,)),
            dma((2,)),
            dma((2,)),
            dma((1,)),
            dma((1,)),
            dma((2,)),
            dma((2,)),
            dma((F - 1,)),
            dma((F - 1,)),
        ],
        compiler_params=pltpu.CompilerParams(
            collective_id=0, has_side_effects=True, vmem_limit_bytes=67043328
        ),
    )(*arrays)
    return d_input, grad.astype(f32), norms.reshape(-1)


def solution(mesh):
    R, F, T = (mesh.shape[a] for a in ("rep", "fs", "tp"))

    def whole(tokens, mid_tokens, out_grad, gate_first, *rest):
        D, FF = gate_first.shape
        n = tokens.shape[0] // (R * F)
        H = FF // (T * R)
        sizes = (R, F, T, n, D, H, 3 if F <= 8 and H % 384 == 0 else 1)
        body = functools.partial(on_device, sizes)
        if (R, F, T) == (2, 8, 2) and H % 256 == 0 and D % 1024 == 0 and n % 128 == 0:
            body = functools.partial(on_square, (R, F, T, n, D, H // 2))
        return jax.shard_map(
            body,
            mesh=mesh,
            in_specs=(P(("rep", "fs"), None),) * 3 + (P("fs", "tp"), P("fs", "tp"), P("tp", "fs")) * 2,
            out_specs=(P(("rep", "fs"), None), P("tp", "fs"), P("tp")),
            check_vma=False,
        )(tokens, mid_tokens, out_grad, gate_first, *rest)

    return whole
```
